128 devices in a mesh: ep: 32 (over z, y, core), tp: 4 (over x).
Axes of the slice: x: 4, y: 4, z: 4, core: 2. Of those that a mesh axis runs over, the one named last changes fastest.
Arguments:
- queries: bfloat16 [16384, 1024], P('ep', 'tp'), may hold values from -6 to 6
- keys: bfloat16 [16384, 512], P('ep', 'tp'), may hold values from -6 to 6
- values: bfloat16 [16384, 512], P('ep', 'tp'), may hold values from -384 to 384
- query_gain: float32 [128], replicated, may hold values from 0.1 to 1.9
- key_gain: float32 [128], replicated, may hold values from 0.1 to 1.9
- out_proj: bfloat16 [1024, 2048], replicated, may hold values from -0.1875 to 0.1875
- tokens_b: bfloat16 [16384, 2048], P(('ep', 'tp')), may hold values from -6 to 6
- norm_gain: float32 [2048], replicated, may hold values from 0.1 to 1.9
- routes: int32 [16384, 2], P(('ep', 'tp')), may hold values from 0 to 127, all different within a row; in each aligned block of 128 rows (0 to 127, 128 to 255, ...) at most 4 rows name the same one
- group_prob: float32 [16384], P(('ep', 'tp')), may hold values from 0.25 to 1
- expert_logits: float32 [16384, 2], P(('ep', 'tp')), may hold values from -6 to 6
- w_gate: bfloat16 [128, 2048, 512], P(('ep', 'tp')), may hold values from -0.125 to 0.125
- w_up: bfloat16 [128, 2048, 512], P(('ep', 'tp')), may hold values from -0.125 to 0.125
- w_down: bfloat16 [128, 512, 2048], P(('ep', 'tp')), may hold values from -0.25 to 0.25
Outputs:
- mixed_a: bfloat16 [16384, 2048], P(('ep', 'tp'))
- mixed_b: bfloat16 [16384, 2048], P(('ep', 'tp'))
The draws below stay inside these ranges and needn't reach their ends.
Inputs may be any that keep to these rules, and one draw needn't show every extreme that they name: Within the 128 rows of one device, no expert is named by more than 4 of the routes, and in every draw some expert is named exactly 4 times by the rows of some device. The 2 experts of a row differ.
All inputs are finite; a program needn't handle non-finite values.
Results may differ from the reference program's by a relative error of at most 0.014.
Values may be sent and summed in bfloat16 or wider, within the bound.
A program may use at most 128 MiB of HBM per device.

```python
import math
import jax
import jax.numpy as jnp
import numpy as np
from jax import lax

D = 2048
HEADS = 8
KV_HEADS = 4
HD = 128
FF_E = 512
GRID_W = 64
TOP_K = 2
TOK_B = 128
SEQ = 16384
TOKENS_B = 16384
EXPERTS = 128
CAP = 4
N_EP = 32
N_TP = 4


def levels(own_key, dims, split, low, high):
    level, own = 1.0, jax.random.fold_in(own_key, 6)
    for axis_at, blocks in split:
        heights = jnp.exp(jax.random.uniform(jax.random.fold_in(own, axis_at), (blocks,), jnp.float32, low / len(split), high / len(split)))
        level = level * jnp.repeat(heights, dims[axis_at] // blocks).reshape([-1 if axis == axis_at else 1 for axis in range(len(dims))])
    return level


def assign_block(key, own, number, rows, number_of, top, bound, lean):
    sequence = jax.random.permutation(key, number_of)
    packed, common = portions_of(number_of, rows * top, bound, lean, True), portions_of(number_of, rows * top, bound, lean, False)
    places = jnp.arange(number_of)

    def named(sizes, turn):
        used = int((sizes > 0).sum())
        fixed = max(1, used // 4)
        moved = fixed + (places - fixed + turn * (used - fixed)) % max(1, number_of - fixed)
        return jnp.zeros((number_of,), jnp.int32).at[sequence[jnp.where(places < fixed, places, moved)]].set(jnp.asarray(sizes, jnp.int32))

    sizes = jnp.where(number % 4 == 0, named(packed, number // 4), named(common, number - number // 4 - 1))
    mixed = jax.random.permutation(jax.random.fold_in(own, 3), number_of)
    source_of, receiver = mixed[0:number_of // 2 * 2:2], mixed[1:number_of // 2 * 2:2]
    slack = jnp.minimum(sizes[source_of] - 1, bound - sizes[receiver]) // 2
    slack = jnp.where((source_of == sequence[0]) | (receiver == sequence[0]) | (sizes[receiver] == 0), 0, jnp.maximum(slack, 0))
    moved = jax.random.randint(jax.random.fold_in(own, 4), (number_of // 2,), 0, 1 << 20) % (slack + 1)
    sizes = sizes.at[source_of].add(-moved).at[receiver].add(moved)
    members = jnp.searchsorted(jnp.cumsum(sizes), jnp.arange(rows * top), side="right").astype(jnp.int32)
    table = members.reshape(top, rows).T
    table = table[jax.random.permutation(jax.random.fold_in(own, 1), rows)]
    turn = jax.random.randint(jax.random.fold_in(own, 2), (rows, 1), 0, top)
    return jnp.take_along_axis(table, (jnp.arange(top)[None, :] + turn) % top, axis=1)


def portions_of(number_of, total, limit, skew, full):
    portions = [(1 << 20) // math.isqrt(standing ** skew) + 1 for standing in range(1, number_of + 1)]
    largest = limit if full else min(limit, max(-(-total // number_of), total * portions[0] // sum(portions)))
    least = 1 if total - largest >= number_of - 1 else 0
    given, spare = [largest] + [least] * (number_of - 1), total - largest - least * (number_of - 1)
    while spare > 0:
        movable = [i for i in range(1, number_of) if given[i] < largest] or [i for i in range(1, number_of) if given[i] < limit]
        pool, left = sum([portions[i] for i in movable]), spare
        for i in movable:
            more = min(limit - given[i], max(1, left * portions[i] // pool), spare)
            given[i] = given[i] + more
            spare = spare - more
    return np.array(given)


def bell_draw(own_key, dims, scale, most, pieces=(), kind=jnp.bfloat16):
    loudness = levels(own_key, dims, pieces, -0.22, 0.18) if pieces else 1.0
    array = jax.random.normal(own_key, dims, jnp.float32) * scale * loudness
    return jnp.minimum(jnp.maximum(array, -most), most).astype(kind)


def setup_inputs(seed: int = 0) -> dict:
    splits = jax.random.split(jax.random.key(seed), 15)
    queries = bell_draw(splits[0], (SEQ, HEADS * HD), 1.0, 6.0, ((0, 32), (1, 4)))
    keys = bell_draw(splits[1], (SEQ, KV_HEADS * HD), 1.0, 6.0, ((0, 32), (1, 4)))
    values = bell_draw(splits[2], (SEQ, KV_HEADS * HD), 64.0, 384.0, ((0, 32), (1, 4)))
    query_gain = jnp.clip(1.0 + 0.18 * jax.random.normal(splits[3], (HD,), jnp.float32), 0.1, 1.9)
    key_gain = jnp.clip(1.0 + 0.18 * jax.random.normal(splits[4], (HD,), jnp.float32), 0.1, 1.9)
    out_proj = bell_draw(splits[5], (HEADS * HD, D), (HEADS * HD) ** -0.5, 0.1875)
    tokens_b = bell_draw(splits[6], (TOKENS_B, D), 1.0, 6.0, ((0, 128),))
    norm_gain = jnp.clip(1.0 + 0.18 * jax.random.normal(splits[7], (D,), jnp.float32), 0.1, 1.9)
    routes_keys = jax.random.split(jax.random.fold_in(splits[8], 1), TOKENS_B // TOK_B)
    routes_turns = jax.random.permutation(jax.random.fold_in(splits[8], 3), TOKENS_B // TOK_B)
    routes = jax.vmap(lambda own, number: assign_block(jax.random.fold_in(splits[8], 2), own, number, TOK_B, EXPERTS, TOP_K, CAP, 1))(routes_keys, routes_turns).reshape((TOKENS_B, TOP_K))
    group_prob = jnp.clip(0.25 + 0.75 * jax.random.uniform(splits[9], (TOKENS_B,), jnp.float32) ** levels(splits[9], (TOKENS_B,), ((0, 128),), -0.2, 0.2), 0.25, 1.0)
    expert_logits = bell_draw(splits[10], (TOKENS_B, TOP_K), 1.5, 6.0, ((0, 128),), jnp.float32)
    w_gate = bell_draw(splits[11], (EXPERTS, D, FF_E), D ** -0.5, 0.125, ((0, 128),))
    w_up = bell_draw(splits[12], (EXPERTS, D, FF_E), D ** -0.5, 0.125, ((0, 128),))
    w_down = bell_draw(splits[13], (EXPERTS, FF_E, D), FF_E ** -0.5, 0.25, ((0, 128),))
    return {"queries": queries, "keys": keys, "values": values, "query_gain": query_gain, "key_gain": key_gain, "out_proj": out_proj, "tokens_b": tokens_b, "norm_gain": norm_gain, "routes": routes, "group_prob": group_prob, "expert_logits": expert_logits, "w_gate": w_gate, "w_up": w_up, "w_down": w_down}


NORM_EPS = 1e-06
ROPE_BASE = 10000.0

def rope_angles(row_count, offset, head_dim):
    quarter = head_dim // 4
    position = offset + jnp.arange(row_count, dtype=jnp.int32)
    grid_row = (position // GRID_W).astype(jnp.float32)
    grid_col = (position % GRID_W).astype(jnp.float32)
    frequency = ROPE_BASE ** (-jnp.arange(quarter, dtype=jnp.float32) / quarter)
    angles = jnp.concatenate([grid_row[:, None] * frequency, grid_col[:, None] * frequency], axis=1)
    return (jnp.cos(angles), jnp.sin(angles))

def norm_rotate(block_in, gain, cos_table, sin_table):
    wide = block_in.astype(jnp.float32)
    wide = wide * lax.rsqrt(lax.optimization_barrier(jnp.mean(wide * wide, axis=-1, keepdims=True)) + NORM_EPS) * gain
    half_width = wide.shape[-1] // 2
    first_half, second_half = (wide[..., :half_width], wide[..., half_width:])
    cos_b = cos_table[:, None, :]
    sin_b = sin_table[:, None, :]
    turned = jnp.concatenate([first_half * cos_b - second_half * sin_b, second_half * cos_b + first_half * sin_b], axis=-1)
    return turned.astype(jnp.bfloat16)

def reference(queries, keys, values, query_gain, key_gain, out_proj, tokens_b, norm_gain, routes, group_prob, expert_logits, w_gate, w_up, w_down):
    group_size = HEADS // KV_HEADS
    cos_table, sin_table = rope_angles(SEQ, 0, HD)
    qrot = norm_rotate(queries.reshape(SEQ, HEADS, HD), query_gain, cos_table, sin_table)
    qrot = qrot.reshape(SEQ, KV_HEADS, group_size, HD)
    krot = norm_rotate(keys.reshape(SEQ, KV_HEADS, HD), key_gain, cos_table, sin_table).astype(jnp.float32)
    value_heads = values.reshape(SEQ, KV_HEADS, HD).astype(jnp.float32)
    query_block = math.gcd(SEQ, 256)

    def one_block(row_start):
        chosen = lax.dynamic_slice_in_dim(qrot, row_start, query_block, 0).astype(jnp.float32)
        scores = jnp.einsum('qhgd,khd->qhgk', chosen, krot) * HD ** (-0.5)
        weights = jnp.exp(scores).astype(jnp.bfloat16).astype(jnp.float32)
        denominator = lax.optimization_barrier(jnp.sum(weights, axis=-1))
        numerator = jnp.einsum('qhgk,khd->qhgd', weights, value_heads)
        return (numerator / denominator[..., None]).astype(jnp.bfloat16)
    starts = (jnp.arange(SEQ // query_block, dtype=jnp.int32) * query_block).astype(jnp.int32)
    attended = lax.map(one_block, starts).reshape(SEQ, HEADS * HD)
    mixed_a = jnp.dot(attended, out_proj, preferred_element_type=jnp.float32).astype(jnp.bfloat16)
    wide_b = tokens_b.astype(jnp.float32)
    normed = (wide_b * lax.rsqrt(lax.optimization_barrier(jnp.mean(wide_b * wide_b, axis=-1, keepdims=True)) + NORM_EPS) * norm_gain).astype(jnp.bfloat16)
    combine = group_prob[:, None] * jax.nn.softmax(expert_logits, axis=-1)
    combine_flat = combine.reshape(-1)
    device_count = N_EP * N_TP
    per_device = TOK_B * TOP_K
    flat_routes = routes.reshape(device_count, per_device)
    onehot = (flat_routes[:, :, None] == jnp.arange(EXPERTS, dtype=jnp.int32)[None, None, :]).astype(jnp.int32)
    slot_rank = lax.optimization_barrier(jnp.sum((jnp.cumsum(onehot, axis=1) - onehot) * onehot, axis=2)).astype(jnp.int32)
    source = jnp.broadcast_to(jnp.arange(device_count, dtype=jnp.int32)[:, None], (device_count, per_device))
    assign_ids = (source * per_device + jnp.arange(per_device, dtype=jnp.int32)[None, :]).astype(jnp.int32)
    slot_table = jnp.zeros((EXPERTS, device_count, CAP), jnp.int32).at[flat_routes, source, slot_rank].set(assign_ids + 1)
    slot_table = slot_table.reshape(EXPERTS, device_count * CAP)

    def per_expert(accumulated, expert_args):
        slot_ids, gate_w, up_w, down_w = expert_args
        live_slots = slot_ids > 0
        assign = jnp.maximum(slot_ids - 1, 0).astype(jnp.int32)
        token_index = (assign // TOP_K).astype(jnp.int32)
        inputs = jnp.where(live_slots[:, None], normed[token_index], jnp.zeros((), jnp.bfloat16))
        gate_part = jnp.dot(inputs, gate_w, preferred_element_type=jnp.float32)
        up_part = jnp.dot(inputs, up_w, preferred_element_type=jnp.float32)
        hidden = (jax.nn.silu(gate_part) * up_part).astype(jnp.bfloat16)
        expert_out = jnp.dot(hidden, down_w, preferred_element_type=jnp.float32).astype(jnp.bfloat16)
        factor = jnp.where(live_slots, combine_flat[assign], jnp.zeros((), jnp.float32))
        return (accumulated.at[token_index].add(factor[:, None] * expert_out.astype(jnp.float32)), None)
    accumulated = lax.scan(per_expert, jnp.zeros((TOKENS_B, D), jnp.float32), (slot_table, w_gate, w_up, w_down))[0]
    mixed_b = accumulated.astype(jnp.bfloat16)
    return (mixed_a, mixed_b)
```

```python
import functools

import jax
import jax.numpy as jnp
import numpy as np
from jax import lax
from jax.experimental import pallas as pl
from jax.experimental.pallas import tpu as pltpu
from jax.sharding import PartitionSpec as P

GRID_W = 64
NORM_EPS = 1e-06
ROPE_BASE = 10000.0
HD = 128
CAP = 4
N_DEV = 128
ROWS = 512
TOK = 128
D = 2048
FF = 512
SEQ = 16384
SCALE_LOG2E = float(HD**-0.5 * np.log2(np.e))
KEY_BLOCK = 2048
MESH = pl.DeviceIdType.MESH
VMEM = pl.BlockSpec(memory_space=pltpu.VMEM)
ANY = pl.BlockSpec(memory_space=pl.ANY)


def angle_tables():
    quarter = HD // 4
    freq = (ROPE_BASE ** (-np.arange(quarter, dtype=np.float64) / quarter)).astype(np.float32)

    def pair(count, at):
        angles = np.arange(count, dtype=np.float32)[:, None] * freq[None, :]
        cos = np.zeros((count, HD), np.float32)
        sin = np.zeros((count, HD), np.float32)
        c, s = np.cos(angles.astype(np.float64)), np.sin(angles.astype(np.float64))
        cos[:, at : at + quarter] = c
        cos[:, 64 + at : 64 + at + quarter] = c
        sin[:, at : at + quarter] = -s
        sin[:, 64 + at : 64 + at + quarter] = s
        return cos, sin

    return pair(SEQ // GRID_W, 0) + pair(GRID_W, quarter)


def prep_kernel(
    q_ref, k_ref, v_ref, qg_ref, kg_ref, rc_ref, rs_ref, cc_ref, cs_ref,
    tok_ref, ng_ref, routes_ref, gp_ref, lg_ref,
    rows_ref, kv_ref, qr_ref, c0_ref, c1_ref, w_ref,
):
    f32, bf16 = jnp.float32, jnp.bfloat16
    wide = tok_ref[...].astype(f32)
    normed = (
        wide * lax.rsqrt(jnp.mean(wide * wide, axis=-1, keepdims=True) + NORM_EPS) * ng_ref[...]
    ).astype(bf16)
    lane = lax.broadcasted_iota(jnp.int32, (TOK, N_DEV), 1)
    sub = lax.broadcasted_iota(jnp.int32, (TOK, N_DEV), 0)
    r0, r1 = routes_ref[:, 0:1], routes_ref[:, 1:2]
    hot0 = (lane == r0).astype(f32)
    hot1 = (lane == r1).astype(f32)
    before = (sub > lane).astype(bf16)
    count0 = jnp.dot(before, hot0.astype(bf16), preferred_element_type=f32)
    count1 = jnp.dot(before, hot1.astype(bf16), preferred_element_type=f32)
    count1 = count1 + jnp.sum(hot0, axis=0, keepdims=True)
    rank0 = jnp.sum(count0 * hot0, axis=1, keepdims=True)
    rank1 = jnp.sum(count1 * hot1, axis=1, keepdims=True)
    slot0 = r0 * CAP + rank0.astype(jnp.int32)
    slot1 = r1 * CAP + rank1.astype(jnp.int32)
    slots = lax.broadcasted_iota(jnp.int32, (TOK, N_DEV * CAP), 1)
    c0 = (slots == slot0).astype(f32)
    c1 = (slots == slot1).astype(f32)
    c0_ref[...] = c0.astype(bf16)
    c1_ref[...] = c1.astype(bf16)
    picked = lax.dot_general(
        (c0 + c1).astype(bf16), normed, (((0,), (0,)), ((), ())), preferred_element_type=f32
    ).astype(bf16)
    rows_ref[...] = picked.reshape(N_DEV, CAP, D)

    l0, l1 = lg_ref[:, 0:1], lg_ref[:, 1:2]
    top = jnp.maximum(l0, l1)
    e0, e1 = jnp.exp(l0 - top), jnp.exp(l1 - top)
    prob = jnp.sum(jnp.where(sub == lane, gp_ref[...], 0.0), axis=1, keepdims=True)
    w_ref[:, 0:1] = prob * (e0 / (e0 + e1))
    w_ref[:, 1:2] = prob * (e1 / (e0 + e1))

    ep = lax.axis_index("ep")
    grid_rows = ROWS // GRID_W
    here = pl.ds(pl.multiple_of(ep * grid_rows, grid_rows), grid_rows)
    cos = (rc_ref[here, :][:, None, :] + cc_ref[...][None, :, :]).reshape(ROWS, HD)
    sin = (rs_ref[here, :][:, None, :] + cs_ref[...][None, :, :]).reshape(ROWS, HD)

    def turned(x, gain):
        x = x.astype(f32)
        x = x * lax.rsqrt(jnp.mean(x * x, axis=-1, keepdims=True) + NORM_EPS) * gain
        return (x * cos + pltpu.roll(x, 64, 1) * sin).astype(bf16)

    kv_ref[:, :HD] = turned(k_ref[...], kg_ref[...])
    kv_ref[:, HD:] = v_ref[...]
    qr_ref[:ROWS] = turned(q_ref[:, :HD], qg_ref[...])
    qr_ref[ROWS:] = turned(q_ref[:, HD:], qg_ref[...])


def arrivals():
    def of(o1, o2):
        parts = (0, 1) if (o1 == 2 or o2 == 2) else (None,)
        return [(p, o1, o2, part) for p in (0, 1) for part in parts]

    order = []
    for o1, o2 in [
        (-1, 0), (1, 0), (0, -1), (0, 1), (2, 0),
        (-1, -1), (1, 1), (-1, 1), (1, -1), (0, 2),
        (2, -1), (2, 1), (-1, 2), (1, 2), (2, 2),
    ]:
        order += of(o1, o2)
    return order


ARRIVALS = arrivals()
SEM_OF = {a: i for i, a in enumerate(ARRIVALS)}


def main_kernel(
    rows_ref, kv_ref, qr_ref, c0_ref, c1_ref, w_ref, wg_hbm, wu_hbm, wd_hbm, op_hbm,
    a_ref, b_ref,
    kvbuf, arrived, sent, ret, acc, att_out, att_in, wg, wu, wd, op,
    w_sem, disp_send, disp_recv, ret_send, ret_recv, kv_send, kv_recv, d2d_send, d2d_recv,
    att_send, att_recv,
):
    f32, bf16 = jnp.float32, jnp.bfloat16
    ep, tp = lax.axis_index("ep"), lax.axis_index("tp")
    z, y, c = ep // 8, (ep // 2) % 4, ep % 2
    me = ep * 4 + tp
    g = (tp + y + z) % 4
    partner = ep + 1 - 2 * c

    loads = [
        pltpu.make_async_copy(wg_hbm.at[0], wg, w_sem.at[0]),
        pltpu.make_async_copy(wu_hbm.at[0], wu, w_sem.at[1]),
        pltpu.make_async_copy(wd_hbm.at[0], wd, w_sem.at[2]),
        pltpu.make_async_copy(op_hbm, op, w_sem.at[3]),
    ]
    for load in loads:
        load.start()

    def remote(src, dst, send, recv, to):
        return pltpu.make_async_remote_copy(
            src_ref=src, dst_ref=dst, send_sem=send, recv_sem=recv,
            device_id=to, device_id_type=MESH,
        )

    barrier = pltpu.get_barrier_semaphore()

    def greet(k, _):
        to = (ep ^ (k // 4), tp ^ (k % 4))
        pl.semaphore_signal(barrier, 1, device_id=to, device_id_type=MESH)
        return 0

    lax.fori_loop(1, N_DEV, greet, 0)

    own_rows = pl.ds(pl.multiple_of(ep * ROWS, ROWS), ROWS)
    kvbuf[own_rows, :] = kv_ref[...]
    arrived[g * 32 + ep] = rows_ref[me]
    pl.semaphore_wait(barrier, N_DEV - 1)

    def moved(p, ring, step):
        if (ring == 0) == (p == 0):
            return ((z * 4 + (y + step + 4) % 4) * 2 + c, tp)
        return ((((z + step + 4) % 4) * 4 + y) * 2 + c, tp)

    def owner_rows(p, o1, o2, part):
        dy, dz = (o1, o2) if p == 0 else (o2, o1)
        owner = (((z + dz + 4) % 4) * 4 + (y + dy + 4) % 4) * 2 + c
        start = owner * ROWS + p * 256 + (0 if part is None else part * 128)
        size = 256 if part is None else 128
        return pl.ds(pl.multiple_of(start, 128), size)

    def kv_copy(p, o1, o2, part, arrival, to, src=None):
        where = owner_rows(p, o1, o2, part)
        return remote(
            kvbuf.at[where] if src is None else src,
            kvbuf.at[where], kv_send, kv_recv.at[SEM_OF[arrival]], to,
        )

    def to_partner(p, o1, o2, part, sem, src=None):
        where = owner_rows(p, o1, o2, part)
        return remote(
            kvbuf.at[where] if src is None else src,
            kvbuf.at[where], d2d_send, d2d_recv.at[sem], (partner, tp),
        )

    def start_own():
        for p in (0, 1):
            half = kv_ref.at[pl.ds(p * 256, 256)]
            for ring in (0, 1):
                for step in (1, -1):
                    arrival = (p, -step, 0, None) if ring == 0 else (p, 0, -step, None)
                    kv_copy(p, 0, 0, None, arrival, moved(p, ring, step), half).start()
        for p in (0, 1):
            half = kv_ref.at[pl.ds(p * 256, 256)]
            to_partner(p, 0, 0, None, len(ARRIVALS) + p, half).start()

    def relay(a):
        p, o1, o2, part = a
        kv_copy(p, o1, o2, part, a, (partner, tp)).wait_recv()
        if o2 == 0 and o1 in (-1, 1):
            half = 0 if o1 == -1 else 1
            kv_copy(p, o1, 0, half, (p, 2, 0, half), moved(p, 0, -o1)).start()
        if o2 == 0:
            for step in (1, -1):
                kv_copy(p, o1, 0, part, (p, o1, -step, part), moved(p, 1, step)).start()
        if o2 in (-1, 1):
            half = 0 if o2 == -1 else 1
            if part is None or part == half:
                kv_copy(p, o1, o2, half, (p, o1, 2, half), moved(p, 1, -o2)).start()
        to_partner(p, o1, o2, part, SEM_OF[a]).start()

    def dispatch(jd, first, last):
        def send(m, _):
            k = (m * 11) % 32
            z2, y2, c2 = (z + k // 8) % 4, (y + (k // 2) % 4) % 4, (c + k % 2) % 2
            x2 = (g + jd + 8 - y2 - z2) % 4
            e2 = (z2 * 4 + y2) * 2 + c2
            remote(
                rows_ref.at[e2 * 4 + x2], arrived.at[g * 32 + ep],
                disp_send, disp_recv.at[(4 - jd) % 4], (e2, x2),
            ).start()
            return 0

        lax.fori_loop(first, last, send, 0)

    def experts(j):
        count = 31 if j == 0 else 32
        span = pl.ds(0, count)
        remote(
            rows_ref.at[span], arrived.at[span], disp_send, disp_recv.at[j], (partner, tp)
        ).wait_recv()
        group = (g + j) % 4
        at = pl.ds(pl.multiple_of(group * 32, 32), 32)
        x = arrived[at].reshape(32 * CAP, D)
        gate = jnp.dot(x, wg[...], preferred_element_type=f32)
        up = jnp.dot(x, wu[...], preferred_element_type=f32)
        hidden = (gate / (1.0 + jnp.exp(-gate)) * up).astype(bf16)
        out = jnp.dot(hidden, wd[...], preferred_element_type=f32).astype(bf16)
        sent[at] = out.reshape(32, CAP, D)

    def give_back(j):
        if j == 0:
            ret[me] = sent[g * 32 + ep]

        def send(m, _):
            k = (m * 11) % 32
            z2, y2, c2 = (z + k // 8) % 4, (y + (k // 2) % 4) % 4, (c + k % 2) % 2
            x2 = (g + j + 8 - y2 - z2) % 4
            e2 = (z2 * 4 + y2) * 2 + c2
            remote(
                sent.at[((g + j) % 4) * 32 + e2], ret.at[me], ret_send, ret_recv, (e2, x2)
            ).start()
            return 0

        lax.fori_loop(1 if j == 0 else 0, 32, send, 0)

    def attend(first, last):
        ones = jnp.ones((KEY_BLOCK, HD), bf16)

        def block(i, _):
            at = pl.ds(pl.multiple_of(i * KEY_BLOCK, KEY_BLOCK), KEY_BLOCK)
            key = kvbuf[at, :HD]
            value = jnp.concatenate([kvbuf[at, HD:], ones], axis=1)
            for t in range(4):
                rows = pl.ds(t * 256, 256)
                s = lax.dot_general(
                    qr_ref[rows], key, (((1,), (1,)), ((), ())), preferred_element_type=f32
                )
                weights = jnp.exp2(s * SCALE_LOG2E).astype(bf16)
                acc[rows] += jnp.dot(weights, value, preferred_element_type=f32)
            return 0

        lax.fori_loop(first, last, block, 0)

    start_own()
    for jd in (0, 3, 2, 1):
        dispatch(jd, 1 if jd == 0 else 0, 32)
    for a in ARRIVALS:
        relay(a)
    for load in loads[:3]:
        load.wait()
    for j in range(4):
        experts(j)
        give_back(j)
    for p in (0, 1):
        to_partner(p, 0, 0, None, len(ARRIVALS) + p).wait_recv()
    for a in ARRIVALS:
        p, o1, o2, part = a
        to_partner(p, o1, o2, part, SEM_OF[a]).wait_recv()
    acc[...] = jnp.zeros_like(acc)
    attend(0, SEQ // KEY_BLOCK)

    for t in range(4):
        for h in range(2):
            part = acc[pl.ds(h * ROWS + t * TOK, TOK)]
            att_out[t, :, h * HD : (h + 1) * HD] = (part[:, :HD] / part[:, HD:]).astype(bf16)
    for step in (1, 2, 3):
        to = (tp + step) % 4
        remote(att_out.at[to], att_in.at[tp], att_send, att_recv, (ep, to)).start()
    att_in[tp] = att_out[tp]
    loads[3].wait()
    span = pl.ds(0, 3)
    remote(att_out.at[span], att_in.at[span], att_send, att_recv, (partner, tp)).wait_recv()
    total = jnp.dot(att_in[0], op[0:256], preferred_element_type=f32)
    for t in range(1, 4):
        total += jnp.dot(att_in[t], op[t * 256 : (t + 1) * 256], preferred_element_type=f32)
    a_ref[...] = total.astype(bf16)

    span = pl.ds(0, N_DEV - 1)
    remote(sent.at[span], ret.at[span], ret_send, ret_recv, (partner, tp)).wait_recv()
    back = ret[...].reshape(N_DEV * CAP, D)
    first = jnp.dot(c0_ref[...], back, preferred_element_type=f32) * w_ref[:, 0:1]
    second = jnp.dot(c1_ref[...], back, preferred_element_type=f32) * w_ref[:, 1:2]
    b_ref[...] = (first + second).astype(bf16)

    remote(rows_ref.at[span], arrived.at[span], disp_send, ret_recv, (partner, tp)).wait_send()
    remote(sent.at[span], ret.at[span], ret_send, ret_recv, (partner, tp)).wait_send()
    remote(
        kvbuf.at[pl.ds(0, 15 * ROWS)], kvbuf.at[pl.ds(0, 15 * ROWS)],
        kv_send, kv_recv.at[0], (partner, tp),
    ).wait_send()
    remote(
        kvbuf.at[pl.ds(0, 16 * ROWS)], kvbuf.at[pl.ds(0, 16 * ROWS)],
        d2d_send, d2d_recv.at[0], (partner, tp),
    ).wait_send()
    three = pl.ds(0, 3)
    remote(att_out.at[three], att_in.at[three], att_send, att_recv, (partner, tp)).wait_send()


def body(
    queries, keys, values, query_gain, key_gain, out_proj, tokens_b, norm_gain, routes,
    group_prob, expert_logits, w_gate, w_up, w_down,
):
    bf16, f32 = jnp.bfloat16, jnp.float32
    tables = [jnp.asarray(t) for t in angle_tables()]
    out = jax.ShapeDtypeStruct
    rows, kv, qr, c0, c1, weight = pl.pallas_call(
        prep_kernel,
        out_shape=(
            out((N_DEV, CAP, D), bf16),
            out((ROWS, 2 * HD), bf16),
            out((2 * ROWS, HD), bf16),
            out((TOK, N_DEV * CAP), bf16),
            out((TOK, N_DEV * CAP), bf16),
            out((TOK, 2), f32),
        ),
        in_specs=[VMEM] * 14,
        out_specs=(VMEM,) * 6,
        compiler_params=pltpu.CompilerParams(vmem_limit_bytes=40 << 20),
    )(
        queries, keys, values, query_gain.reshape(1, HD), key_gain.reshape(1, HD), *tables,
        tokens_b, norm_gain.reshape(1, D), routes, group_prob.reshape(1, TOK), expert_logits,
    )
    dma, many = pltpu.SemaphoreType.DMA, len(ARRIVALS)
    return pl.pallas_call(
        main_kernel,
        out_shape=(out((TOK, D), bf16), out((TOK, D), bf16)),
        in_specs=[VMEM] * 6 + [ANY] * 4,
        out_specs=(VMEM, VMEM),
        scratch_shapes=[
            pltpu.VMEM((SEQ, 2 * HD), bf16),
            pltpu.VMEM((N_DEV, CAP, D), bf16),
            pltpu.VMEM((N_DEV, CAP, D), bf16),
            pltpu.VMEM((N_DEV, CAP, D), bf16),
            pltpu.VMEM((2 * ROWS, 2 * HD), f32),
            pltpu.VMEM((4, TOK, 2 * HD), bf16),
            pltpu.VMEM((4, TOK, 2 * HD), bf16),
            pltpu.VMEM((D, FF), bf16),
            pltpu.VMEM((D, FF), bf16),
            pltpu.VMEM((FF, D), bf16),
            pltpu.VMEM((8 * HD, D), bf16),
            dma((4,)), dma, dma((4,)), dma, dma, dma, dma((many,)), dma, dma((many + 2,)),
            dma, dma,
        ],
        compiler_params=pltpu.CompilerParams(
            collective_id=0, has_side_effects=True, vmem_limit_bytes=60 << 20
        ),
    )(rows, kv, qr, c0, c1, weight, w_gate, w_up, w_down, out_proj)


def solution(mesh):
    both = P(("ep", "tp"), None)
    placed = (
        P("ep", "tp"),
        P("ep", "tp"),
        P("ep", "tp"),
        P(),
        P(),
        P(),
        both,
        P(),
        both,
        P(("ep", "tp")),
        both,
        P(("ep", "tp"), None, None),
        P(("ep", "tp"), None, None),
        P(("ep", "tp"), None, None),
    )
    return jax.shard_map(
        body, mesh=mesh, in_specs=placed, out_specs=(both, both), check_vma=False
    )
```

```python
import functools

import jax
import jax.numpy as jnp
import numpy as np
from jax import lax
from jax.experimental import pallas as pl
from jax.experimental.pallas import tpu as pltpu
from jax.sharding import PartitionSpec as P

GRID_W = 64
NORM_EPS = 1e-06
ROPE_BASE = 10000.0
HD = 128
CAP = 4
N_DEV = 128
ROWS = 512
TOK = 128
D = 2048
FF = 512
SEQ = 16384
SCALE_LOG2E = float(HD**-0.5 * np.log2(np.e))
KEY_BLOCK = 2048
MESH = pl.DeviceIdType.MESH
VMEM = pl.BlockSpec(memory_space=pltpu.VMEM)
ANY = pl.BlockSpec(memory_space=pl.ANY)
HBM = pl.BlockSpec(memory_space=pltpu.HBM)


def angle_tables():
    quarter = HD // 4
    freq = (ROPE_BASE ** (-np.arange(quarter, dtype=np.float64) / quarter)).astype(np.float32)

    def pair(count, at):
        angles = np.arange(count, dtype=np.float32)[:, None] * freq[None, :]
        cos = np.zeros((count, HD), np.float32)
        sin = np.zeros((count, HD), np.float32)
        c, s = np.cos(angles.astype(np.float64)), np.sin(angles.astype(np.float64))
        cos[:, at : at + quarter] = c
        cos[:, 64 + at : 64 + at + quarter] = c
        sin[:, at : at + quarter] = -s
        sin[:, 64 + at : 64 + at + quarter] = s
        return cos, sin

    return pair(SEQ // GRID_W, 0) + pair(GRID_W, quarter)


def arrivals():
    def of(o1, o2):
        parts = (0, 1) if (o1 == 2 or o2 == 2) else (None,)
        return [(p, o1, o2, part) for p in (0, 1) for part in parts]

    order = []
    for o1, o2 in [
        (-1, 0), (1, 0), (0, -1), (0, 1), (2, 0),
        (-1, -1), (1, 1), (-1, 1), (1, -1), (0, 2),
        (2, -1), (2, 1), (-1, 2), (1, 2), (2, 2),
    ]:
        order += of(o1, o2)
    return order


ARRIVALS = arrivals()
SEM_OF = {a: i for i, a in enumerate(ARRIVALS)}

SCHEDULE = (
    ("rows", 0),
    ("relay", 1),
    ("rows", 1),
    ("relay", 2),
    ("rows", 2),
    ("queries", 0),
    ("relay", 3),
    ("rows", 3),
    ("attend", 0),
    ("relay", 4),
    ("experts", 0),
    ("experts", 1),
    ("experts", 2),
    ("experts", 3),
    ("attend", 1),
    ("attend", -1),
    ("attend", 2),
)


def main_kernel(
    q_hbm, k_hbm, v_hbm, qg_hbm, kg_hbm, rc_hbm, rs_hbm, cc_hbm, cs_hbm,
    tok_hbm, ng_hbm, routes_hbm, gp_hbm, lg_hbm, wg_hbm, wu_hbm, wd_hbm, op_hbm,
    a_hbm, b_hbm,
    q_ref, k_ref, qg_ref, kg_ref, rc_ref, rs_ref, cc_ref, cs_ref,
    tok_ref, ng_ref, routes_ref, gp_ref, lg_ref,
    rows_ref, qr_ref, pick_ref, w_ref, a_buf, b_buf, b_sum,
    kvbuf, arrived, sent, ret, acc, att_out, att_in, wg, wu, wd, op,
    w_sem, in_sem, disp_send, disp_recv, ret_send, ret_recv,
    kv_send, kv_recv, d2d_send, d2d_recv, att_send, att_recv,
):
    f32, bf16 = jnp.float32, jnp.bfloat16
    ep, tp = lax.axis_index("ep"), lax.axis_index("tp")
    z, y, c = ep // 8, (ep // 2) % 4, ep % 2
    g = (tp + y + z) % 4
    me = g * 32 + ep
    partner = ep + 1 - 2 * c
    own_rows = pl.ds(pl.multiple_of(ep * ROWS, ROWS), ROWS)
    grid_rows = ROWS // GRID_W
    here = pl.ds(pl.multiple_of(ep * grid_rows, grid_rows), grid_rows)

    barrier = pltpu.get_barrier_semaphore()

    def greet(k, _):
        to = (ep ^ (k // 4), tp ^ (k % 4))
        pl.semaphore_signal(barrier, 1, device_id=to, device_id_type=MESH)
        return 0

    lax.fori_loop(1, N_DEV, greet, 0)

    takes = [
        (k_hbm, k_ref), (kg_hbm, kg_ref), (rc_hbm.at[here], rc_ref), (rs_hbm.at[here], rs_ref),
        (cc_hbm, cc_ref), (cs_hbm, cs_ref), (v_hbm, kvbuf.at[own_rows, pl.ds(HD, HD)]),
        (q_hbm, q_ref), (qg_hbm, qg_ref),
        (tok_hbm, tok_ref), (ng_hbm, ng_ref), (routes_hbm, routes_ref), (gp_hbm, gp_ref),
        (lg_hbm, lg_ref),
    ]
    takes = [pltpu.make_async_copy(x, to, in_sem.at[i]) for i, (x, to) in enumerate(takes)]
    for take in takes:
        take.start()

    loads = [
        pltpu.make_async_copy(wg_hbm.at[0], wg, w_sem.at[0]),
        pltpu.make_async_copy(wu_hbm.at[0], wu, w_sem.at[1]),
        pltpu.make_async_copy(wd_hbm.at[0], wd, w_sem.at[2]),
        pltpu.make_async_copy(op_hbm, op, w_sem.at[3]),
    ]
    def remote(src, dst, send, recv, to):
        return pltpu.make_async_remote_copy(
            src_ref=src, dst_ref=dst, send_sem=send, recv_sem=recv,
            device_id=to, device_id_type=MESH,
        )

    for take in takes[:7]:
        take.wait()
    cos = (rc_ref[...][:, None, :] + cc_ref[...][None, :, :]).reshape(ROWS, HD)
    sin = (rs_ref[...][:, None, :] + cs_ref[...][None, :, :]).reshape(ROWS, HD)

    def turned(x, gain):
        x = x.astype(f32)
        x = x * lax.rsqrt(jnp.mean(x * x, axis=-1, keepdims=True) + NORM_EPS) * gain
        return (x * cos + pltpu.roll(x, 64, 1) * sin).astype(bf16)

    kvbuf[own_rows, :HD] = turned(k_ref[...], kg_ref[...])
    pl.semaphore_wait(barrier, N_DEV - 1)
    def moved(p, ring, step):
        if (ring == 0) == (p == 0):
            return ((z * 4 + (y + step + 4) % 4) * 2 + c, tp)
        return ((((z + step + 4) % 4) * 4 + y) * 2 + c, tp)

    def owner_rows(p, o1, o2, part):
        dy, dz = (o1, o2) if p == 0 else (o2, o1)
        owner = (((z + dz + 4) % 4) * 4 + (y + dy + 4) % 4) * 2 + c
        start = owner * ROWS + p * 256 + (0 if part is None else part * 128)
        size = 256 if part is None else 128
        return pl.ds(pl.multiple_of(start, 128), size)

    def kv_copy(p, o1, o2, part, arrival, to):
        at = kvbuf.at[owner_rows(p, o1, o2, part)]
        return remote(at, at, kv_send, kv_recv.at[SEM_OF[arrival]], to)

    def to_partner(p, o1, o2, part, sem):
        at = kvbuf.at[owner_rows(p, o1, o2, part)]
        return remote(at, at, d2d_send, d2d_recv.at[sem], (partner, tp))

    def start_own():
        for p in (0, 1):
            for ring in (0, 1):
                for step in (1, -1):
                    arrival = (p, -step, 0, None) if ring == 0 else (p, 0, -step, None)
                    kv_copy(p, 0, 0, None, arrival, moved(p, ring, step)).start()
        for p in (0, 1):
            to_partner(p, 0, 0, None, len(ARRIVALS) + p).start()

    def relay(a):
        p, o1, o2, part = a
        kv_copy(p, o1, o2, part, a, (partner, tp)).wait_recv()
        if o2 == 0 and o1 in (-1, 1):
            half = 0 if o1 == -1 else 1
            kv_copy(p, o1, 0, half, (p, 2, 0, half), moved(p, 0, -o1)).start()
        if o2 == 0:
            for step in (1, -1):
                kv_copy(p, o1, 0, part, (p, o1, -step, part), moved(p, 1, step)).start()
        if o2 in (-1, 1):
            half = 0 if o2 == -1 else 1
            if part is None or part == half:
                kv_copy(p, o1, o2, half, (p, o1, 2, half), moved(p, 1, -o2)).start()
        to_partner(p, o1, o2, part, SEM_OF[a]).start()

    def pick_rows():
        for take in takes[9:]:
            take.wait()
        lane = lax.broadcasted_iota(jnp.int32, (TOK, N_DEV), 1)
        sub = lax.broadcasted_iota(jnp.int32, (TOK, N_DEV), 0)
        diagonal = sub == lane

        def column(row):
            return jnp.sum(jnp.where(diagonal, row, 0.0), axis=1, keepdims=True)

        wide = tok_ref[...].astype(f32)
        normed = (
            wide * lax.rsqrt(jnp.mean(wide * wide, axis=-1, keepdims=True) + NORM_EPS) * ng_ref[...]
        ).astype(bf16)
        routed = routes_ref[...].astype(f32)
        r0 = column(routed[0:1]).astype(jnp.int32)
        r1 = column(routed[1:2]).astype(jnp.int32)
        hot0 = (lane == r0).astype(f32)
        hot1 = (lane == r1).astype(f32)
        before = (sub > lane).astype(f32).astype(bf16)
        count0 = jnp.dot(before, hot0.astype(bf16), preferred_element_type=f32)
        count1 = jnp.dot(before, hot1.astype(bf16), preferred_element_type=f32)
        count1 = count1 + jnp.sum(hot0, axis=0, keepdims=True)
        rank0 = jnp.sum(count0 * hot0, axis=1, keepdims=True)
        rank1 = jnp.sum(count1 * hot1, axis=1, keepdims=True)
        slots = lax.broadcasted_iota(jnp.int32, (TOK, N_DEV * CAP), 1)

        def place(e):
            return (((e & 3) + ((e >> 3) & 3) + (e >> 5)) & 3) * 32 + (e >> 2)

        c0 = (slots == place(r0) * CAP + rank0.astype(jnp.int32)).astype(f32)
        c1 = (slots == place(r1) * CAP + rank1.astype(jnp.int32)).astype(f32)
        pick_ref[:TOK] = c0.astype(bf16)
        pick_ref[TOK:] = c1.astype(bf16)
        picked = lax.dot_general(
            (c0 + c1).astype(bf16), normed, (((0,), (0,)), ((), ())), preferred_element_type=f32
        ).astype(bf16)
        rows_ref[...] = picked.reshape(N_DEV, CAP, D)
        l0, l1 = lg_ref[0:1], lg_ref[1:2]
        top = jnp.maximum(l0, l1)
        e0, e1 = jnp.exp(l0 - top), jnp.exp(l1 - top)
        w_ref[:, 0:1] = column(gp_ref[...] * (e0 / (e0 + e1)))
        w_ref[:, 1:2] = column(gp_ref[...] * (e1 / (e0 + e1)))
        arrived[me] = rows_ref[me]

    def dispatch(jd, first, last):
        def send(m, _):
            k = (m * 11) % 32
            z2, y2, c2 = (z + k // 8) % 4, (y + (k // 2) % 4) % 4, (c + k % 2) % 2
            x2 = (g + jd + 8 - y2 - z2) % 4
            e2 = (z2 * 4 + y2) * 2 + c2
            remote(
                rows_ref.at[((g + jd) % 4) * 32 + e2], arrived.at[me],
                disp_send, disp_recv.at[(4 - jd) % 4], (e2, x2),
            ).start()
            return 0

        lax.fori_loop(first, last, send, 0)

    def experts(j):
        count = 31 if j == 0 else 32
        span = pl.ds(0, count)
        remote(
            rows_ref.at[span], arrived.at[span], disp_send, disp_recv.at[j], (partner, tp)
        ).wait_recv()
        group = (g + j) % 4
        at = pl.ds(pl.multiple_of(group * 32, 32), 32)
        x = arrived[at].reshape(32 * CAP, D)
        gate = jnp.dot(x, wg[...], preferred_element_type=f32)
        up = jnp.dot(x, wu[...], preferred_element_type=f32)
        hidden = (gate / (1.0 + jnp.exp(-gate)) * up).astype(bf16)
        out = jnp.dot(hidden, wd[...], preferred_element_type=f32).astype(bf16)
        sent[at] = out.reshape(32, CAP, D)

    def give_back(j):
        if j == 0:
            ret[me] = sent[me]

        def send(m, _):
            k = (m * 11) % 32
            z2, y2, c2 = (z + k // 8) % 4, (y + (k // 2) % 4) % 4, (c + k % 2) % 2
            x2 = (g + j + 8 - y2 - z2) % 4
            e2 = (z2 * 4 + y2) * 2 + c2
            remote(
                sent.at[((g + j) % 4) * 32 + e2], ret.at[me],
                ret_send, ret_recv.at[(4 - j) % 4], (e2, x2),
            ).start()
            return 0

        lax.fori_loop(1 if j == 0 else 0, 32, send, 0)

    def combine(j):
        count = 31 if j == 0 else 32
        span = pl.ds(0, count)
        remote(
            sent.at[span], ret.at[span], ret_send, ret_recv.at[j], (partner, tp)
        ).wait_recv()
        group = (g + j) % 4
        back = ret[pl.ds(pl.multiple_of(group * 32, 32), 32)].reshape(32 * CAP, D)
        pick = pick_ref[:, pl.ds(pl.multiple_of(group * 128, 128), 128)]
        picked = jnp.dot(pick, back, preferred_element_type=f32)
        part = picked[:TOK] * w_ref[:, 0:1] + picked[TOK:] * w_ref[:, 1:2]
        if j == 0:
            b_sum[...] = part
        else:
            b_sum[...] += part

    ones = jnp.ones((KEY_BLOCK, HD), bf16)

    def attend(dz):
        if dz == 0:
            for p in (0, 1):
                to_partner(p, 0, 0, None, len(ARRIVALS) + p).wait_recv()
        for a in ARRIVALS:
            if (a[2] if a[0] == 0 else a[1]) == dz:
                to_partner(*a, SEM_OF[a]).wait_recv()
        plane = ((z + dz + 4) % 4) * (8 * ROWS)

        def block(i, _):
            at = pl.ds(pl.multiple_of(plane + i * KEY_BLOCK, KEY_BLOCK), KEY_BLOCK)
            key = kvbuf[at, :HD]
            value = jnp.concatenate([kvbuf[at, HD:], ones], axis=1)
            for t in range(4):
                rows = pl.ds(t * 256, 256)
                s = lax.dot_general(
                    qr_ref[rows], key, (((1,), (1,)), ((), ())), preferred_element_type=f32
                )
                weights = jnp.exp2(s * SCALE_LOG2E).astype(bf16)
                acc[rows] += jnp.dot(weights, value, preferred_element_type=f32)
            return 0

        lax.fori_loop(0, 8 * ROWS // KEY_BLOCK, block, 0)

    start_own()
    for load in loads:
        load.start()
    pick_rows()
    for kind, at in SCHEDULE:
        if kind == "queries":
            for take in takes[7:9]:
                take.wait()
            qr_ref[:ROWS] = turned(q_ref[:, :HD], qg_ref[...])
            qr_ref[ROWS:] = turned(q_ref[:, HD:], qg_ref[...])
            acc[...] = jnp.zeros_like(acc)
        elif kind == "rows":
            dispatch((4 - at) % 4, 1 if at == 0 else 0, 32)
        elif kind == "relay":
            for a in ARRIVALS:
                if abs(a[1]) + abs(a[2]) == at:
                    relay(a)
        elif kind == "experts":
            if at == 0:
                for load in loads[:3]:
                    load.wait()
            experts(at)
            give_back(at)
        else:
            attend(at)

    for t in range(4):
        for h in range(2):
            part = acc[pl.ds(h * ROWS + t * TOK, TOK)]
            att_out[t, :, h * HD : (h + 1) * HD] = (part[:, :HD] / part[:, HD:]).astype(bf16)
    for step in (1, 2, 3):
        to = (tp + step) % 4
        remote(att_out.at[to], att_in.at[tp], att_send, att_recv, (ep, to)).start()
    att_in[tp] = att_out[tp]
    for j in (0, 3, 2):
        combine(j)
    loads[3].wait()
    span = pl.ds(0, 3)
    remote(att_out.at[span], att_in.at[span], att_send, att_recv, (partner, tp)).wait_recv()
    total = jnp.dot(att_in[0], op[0:256], preferred_element_type=f32)
    for t in range(1, 4):
        total += jnp.dot(att_in[t], op[t * 256 : (t + 1) * 256], preferred_element_type=f32)
    a_buf[...] = total.astype(bf16)
    out_a = pltpu.make_async_copy(a_buf, a_hbm, w_sem.at[4])
    out_a.start()
    combine(1)
    b_buf[...] = b_sum[...].astype(bf16)
    out_b = pltpu.make_async_copy(b_buf, b_hbm, w_sem.at[5])
    out_b.start()
    span = pl.ds(0, N_DEV - 1)

    remote(
        rows_ref.at[span], arrived.at[span], disp_send, ret_recv.at[0], (partner, tp)
    ).wait_send()
    remote(sent.at[span], ret.at[span], ret_send, ret_recv.at[0], (partner, tp)).wait_send()
    remote(
        kvbuf.at[pl.ds(0, 15 * ROWS)], kvbuf.at[pl.ds(0, 15 * ROWS)],
        kv_send, kv_recv.at[0], (partner, tp),
    ).wait_send()
    remote(
        kvbuf.at[pl.ds(0, 16 * ROWS)], kvbuf.at[pl.ds(0, 16 * ROWS)],
        d2d_send, d2d_recv.at[0], (partner, tp),
    ).wait_send()
    three = pl.ds(0, 3)
    remote(att_out.at[three], att_in.at[three], att_send, att_recv, (partner, tp)).wait_send()
    out_a.wait()
    out_b.wait()


def final_kernel(a_in, b_in, a_out, b_out, held, sem):
    ins = [pltpu.make_async_copy(x, held.at[i], sem.at[i]) for i, x in enumerate((a_in, b_in))]
    outs = [
        pltpu.make_async_copy(held.at[i], x, sem.at[2 + i]) for i, x in enumerate((a_out, b_out))
    ]
    for copy in ins:
        copy.start()
    for i in (0, 1):
        ins[i].wait()
        outs[i].start()
    for copy in outs:
        copy.wait()


def body(
    queries, keys, values, query_gain, key_gain, out_proj, tokens_b, norm_gain, routes,
    group_prob, expert_logits, w_gate, w_up, w_down,
):
    bf16, f32 = jnp.bfloat16, jnp.float32
    tables = [jnp.asarray(t) for t in angle_tables()]
    out, buf = jax.ShapeDtypeStruct, pltpu.VMEM
    dma, many = pltpu.SemaphoreType.DMA, len(ARRIVALS)
    mixed = pl.pallas_call(
        main_kernel,
        out_shape=(out((TOK, D), bf16), out((TOK, D), bf16)),
        in_specs=[ANY] * 18,
        out_specs=(HBM, HBM),
        scratch_shapes=[
            buf((ROWS, 2 * HD), bf16), buf((ROWS, HD), bf16), buf((1, HD), f32), buf((1, HD), f32),
            buf((ROWS // GRID_W, HD), f32), buf((ROWS // GRID_W, HD), f32),
            buf((GRID_W, HD), f32), buf((GRID_W, HD), f32),
            buf((TOK, D), bf16), buf((1, D), f32), buf((2, TOK), jnp.int32), buf((1, TOK), f32),
            buf((2, TOK), f32),
            buf((N_DEV, CAP, D), bf16), buf((2 * ROWS, HD), bf16),
            buf((2 * TOK, N_DEV * CAP), bf16), buf((TOK, 2), f32),
            buf((TOK, D), bf16), buf((TOK, D), bf16), buf((TOK, D), f32),
            buf((SEQ, 2 * HD), bf16),
            buf((N_DEV, CAP, D), bf16), buf((N_DEV, CAP, D), bf16), buf((N_DEV, CAP, D), bf16),
            buf((2 * ROWS, 2 * HD), f32),
            buf((4, TOK, 2 * HD), bf16), buf((4, TOK, 2 * HD), bf16),
            buf((D, FF), bf16), buf((D, FF), bf16), buf((FF, D), bf16), buf((8 * HD, D), bf16),
            dma((6,)), dma((14,)), dma, dma((4,)), dma, dma((4,)),
            dma, dma((many,)), dma, dma((many + 2,)), dma, dma,
        ],
        compiler_params=pltpu.CompilerParams(
            collective_id=0, has_side_effects=True, vmem_limit_bytes=60 << 20
        ),
    )(
        queries, keys, values, query_gain.reshape(1, HD), key_gain.reshape(1, HD), *tables,
        tokens_b, norm_gain.reshape(1, D), routes.T, group_prob.reshape(1, TOK),
        expert_logits.T, w_gate, w_up, w_down, out_proj,
    )
    return pl.pallas_call(
        final_kernel,
        out_shape=(out((TOK, D), bf16), out((TOK, D), bf16)),
        in_specs=[HBM] * 2,
        out_specs=(HBM,) * 2,
        scratch_shapes=[buf((2, TOK, D), bf16), dma((4,))],
        compiler_params=pltpu.CompilerParams(vmem_limit_bytes=60 << 20),
    )(*mixed)


def solution(mesh):
    both = P(("ep", "tp"), None)
    placed = (
        P("ep", "tp"),
        P("ep", "tp"),
        P("ep", "tp"),
        P(),
        P(),
        P(),
        both,
        P(),
        both,
        P(("ep", "tp")),
        both,
        P(("ep", "tp"), None, None),
        P(("ep", "tp"), None, None),
        P(("ep", "tp"), None, None),
    )
    return jax.shard_map(
        body, mesh=mesh, in_specs=placed, out_specs=(both, both), check_vma=False
    )
```

```python
import functools

import jax
import jax.numpy as jnp
import numpy as np
from jax import lax
from jax.experimental import pallas as pl
from jax.experimental.pallas import tpu as pltpu
from jax.sharding import PartitionSpec as P

GRID_W = 64
NORM_EPS = 1e-06
ROPE_BASE = 10000.0
HD = 128
CAP = 4
N_DEV = 128
ROWS = 512
TOK = 128
D = 2048
FF = 512
SEQ = 16384
SCALE_LOG2E = float(HD**-0.5 * np.log2(np.e))
KEY_BLOCK = 2048
MESH = pl.DeviceIdType.MESH
VMEM = pl.BlockSpec(memory_space=pltpu.VMEM)
ANY = pl.BlockSpec(memory_space=pl.ANY)
HBM = pl.BlockSpec(memory_space=pltpu.HBM)


def angle_tables():
    quarter = HD // 4
    freq = (ROPE_BASE ** (-np.arange(quarter, dtype=np.float64) / quarter)).astype(np.float32)

    def pair(count, at):
        angles = np.arange(count, dtype=np.float32)[:, None] * freq[None, :]
        cos = np.zeros((count, HD), np.float32)
        sin = np.zeros((count, HD), np.float32)
        c, s = np.cos(angles.astype(np.float64)), np.sin(angles.astype(np.float64))
        cos[:, at : at + quarter] = c
        cos[:, 64 + at : 64 + at + quarter] = c
        sin[:, at : at + quarter] = -s
        sin[:, 64 + at : 64 + at + quarter] = s
        return cos, sin

    return pair(SEQ // GRID_W, 0) + pair(GRID_W, quarter)


def arrivals():
    def of(o1, o2):
        parts = (0, 1) if (o1 == 2 or o2 == 2) else (None,)
        return [(p, o1, o2, part) for p in (0, 1) for part in parts]

    order = []
    for o1, o2 in [
        (-1, 0), (1, 0), (0, -1), (0, 1), (2, 0),
        (-1, -1), (1, 1), (-1, 1), (1, -1), (0, 2),
        (2, -1), (2, 1), (-1, 2), (1, 2), (2, 2),
    ]:
        order += of(o1, o2)
    return order


ARRIVALS = arrivals()
SEM_OF = {a: i for i, a in enumerate(ARRIVALS)}

SCHEDULE = (
    ("rows", 0),
    ("relay", 1),
    ("rows", 1),
    ("relay", 2),
    ("rows", 2),
    ("queries", 0),
    ("relay", 3),
    ("rows", 3),
    ("attend", 0),
    ("relay", 4),
    ("experts", 0),
    ("experts", 1),
    ("attend", 1),
    ("experts", 2),
    ("experts", 3),
    ("attend", -1),
    ("attend", 2),
)


def main_kernel(
    q_hbm, k_hbm, v_hbm, qg_hbm, kg_hbm, rc_hbm, rs_hbm, cc_hbm, cs_hbm,
    tok_hbm, ng_hbm, routes_hbm, gp_hbm, lg_hbm, wg_hbm, wu_hbm, wd_hbm, op_hbm,
    a_hbm, b_hbm,
    q_ref, k_ref, qg_ref, kg_ref, rc_ref, rs_ref, cc_ref, cs_ref,
    tok_ref, ng_ref, routes_ref, gp_ref, lg_ref,
    rows_ref, qr_ref, pick_ref, w_ref, a_buf, b_buf, b_sum,
    kvbuf, arrived, sent, ret, acc, att_out, att_in, wg, wu, wd, op,
    w_sem, in_sem, disp_send, disp_recv, ret_send, ret_recv,
    kv_send, kv_recv, d2d_send, d2d_recv, att_send, att_recv, round_sem,
):
    f32, bf16 = jnp.float32, jnp.bfloat16
    ep, tp = lax.axis_index("ep"), lax.axis_index("tp")
    z, y, c = ep // 8, (ep // 2) % 4, ep % 2
    g = (tp + y + z) % 4
    me = g * 32 + ep
    partner = ep + 1 - 2 * c
    own_rows = pl.ds(pl.multiple_of(ep * ROWS, ROWS), ROWS)
    grid_rows = ROWS // GRID_W
    here = pl.ds(pl.multiple_of(ep * grid_rows, grid_rows), grid_rows)

    barrier = pltpu.get_barrier_semaphore()

    kin = [(ep, (tp + step) % 4) for step in (1, 3, 2)]
    kin += [((z * 4 + (y + step) % 4) * 2 + c, tp) for step in (1, 3, 2)]
    kin += [((((z + step) % 4) * 4 + y) * 2 + c, tp) for step in (1, 3, 2)]
    kin += [(partner, tp)]

    def tell(sem):
        for to in kin:
            pl.semaphore_signal(sem, 1, device_id=to, device_id_type=MESH)

    tell(barrier)

    takes = [
        (k_hbm, k_ref), (kg_hbm, kg_ref), (rc_hbm.at[here], rc_ref), (rs_hbm.at[here], rs_ref),
        (cc_hbm, cc_ref), (cs_hbm, cs_ref), (v_hbm, kvbuf.at[own_rows, pl.ds(HD, HD)]),
        (q_hbm, q_ref), (qg_hbm, qg_ref),
        (tok_hbm, tok_ref), (ng_hbm, ng_ref), (routes_hbm, routes_ref), (gp_hbm, gp_ref),
        (lg_hbm, lg_ref),
    ]
    takes = [pltpu.make_async_copy(x, to, in_sem.at[i]) for i, (x, to) in enumerate(takes)]
    for take in takes:
        take.start()

    loads = [
        pltpu.make_async_copy(wg_hbm.at[0], wg, w_sem.at[0]),
        pltpu.make_async_copy(wu_hbm.at[0], wu, w_sem.at[1]),
        pltpu.make_async_copy(wd_hbm.at[0], wd, w_sem.at[2]),
        pltpu.make_async_copy(op_hbm, op, w_sem.at[3]),
    ]
    def remote(src, dst, send, recv, to):
        return pltpu.make_async_remote_copy(
            src_ref=src, dst_ref=dst, send_sem=send, recv_sem=recv,
            device_id=to, device_id_type=MESH,
        )

    for take in takes[:7]:
        take.wait()
    cos = (rc_ref[...][:, None, :] + cc_ref[...][None, :, :]).reshape(ROWS, HD)
    sin = (rs_ref[...][:, None, :] + cs_ref[...][None, :, :]).reshape(ROWS, HD)

    def turned(x, gain):
        x = x.astype(f32)
        x = x * lax.rsqrt(jnp.mean(x * x, axis=-1, keepdims=True) + NORM_EPS) * gain
        return (x * cos + pltpu.roll(x, 64, 1) * sin).astype(bf16)

    kvbuf[own_rows, :HD] = turned(k_ref[...], kg_ref[...])
    pl.semaphore_wait(barrier, len(kin))
    tell(round_sem.at[0])

    def moved(p, ring, step):
        if (ring == 0) == (p == 0):
            return ((z * 4 + (y + step + 4) % 4) * 2 + c, tp)
        return ((((z + step + 4) % 4) * 4 + y) * 2 + c, tp)

    def owner_rows(p, o1, o2, part):
        dy, dz = (o1, o2) if p == 0 else (o2, o1)
        owner = (((z + dz + 4) % 4) * 4 + (y + dy + 4) % 4) * 2 + c
        start = owner * ROWS + p * 256 + (0 if part is None else part * 128)
        size = 256 if part is None else 128
        return pl.ds(pl.multiple_of(start, 128), size)

    def kv_copy(p, o1, o2, part, arrival, to):
        at = kvbuf.at[owner_rows(p, o1, o2, part)]
        return remote(at, at, kv_send, kv_recv.at[SEM_OF[arrival]], to)

    def to_partner(p, o1, o2, part, sem):
        at = kvbuf.at[owner_rows(p, o1, o2, part)]
        return remote(at, at, d2d_send, d2d_recv.at[sem], (partner, tp))

    def start_own():
        for p in (0, 1):
            for ring in (0, 1):
                for step in (1, -1):
                    arrival = (p, -step, 0, None) if ring == 0 else (p, 0, -step, None)
                    kv_copy(p, 0, 0, None, arrival, moved(p, ring, step)).start()
        for p in (0, 1):
            to_partner(p, 0, 0, None, len(ARRIVALS) + p).start()

    def relay(a):
        p, o1, o2, part = a
        kv_copy(p, o1, o2, part, a, (partner, tp)).wait_recv()
        if o2 == 0 and o1 in (-1, 1):
            half = 0 if o1 == -1 else 1
            kv_copy(p, o1, 0, half, (p, 2, 0, half), moved(p, 0, -o1)).start()
        if o2 == 0:
            for step in (1, -1):
                kv_copy(p, o1, 0, part, (p, o1, -step, part), moved(p, 1, step)).start()
        if o2 in (-1, 1):
            half = 0 if o2 == -1 else 1
            if part is None or part == half:
                kv_copy(p, o1, o2, half, (p, o1, 2, half), moved(p, 1, -o2)).start()
        to_partner(p, o1, o2, part, SEM_OF[a]).start()

    def pick_rows():
        for take in takes[9:]:
            take.wait()
        lane = lax.broadcasted_iota(jnp.int32, (TOK, N_DEV), 1)
        sub = lax.broadcasted_iota(jnp.int32, (TOK, N_DEV), 0)
        diagonal = sub == lane

        def column(row):
            return jnp.sum(jnp.where(diagonal, row, 0.0), axis=1, keepdims=True)

        wide = tok_ref[...].astype(f32)
        normed = (
            wide * lax.rsqrt(jnp.mean(wide * wide, axis=-1, keepdims=True) + NORM_EPS) * ng_ref[...]
        ).astype(bf16)
        routed = routes_ref[...].astype(f32)
        r0 = column(routed[0:1]).astype(jnp.int32)
        r1 = column(routed[1:2]).astype(jnp.int32)
        hot0 = (lane == r0).astype(f32)
        hot1 = (lane == r1).astype(f32)
        before = (sub > lane).astype(f32).astype(bf16)
        count0 = jnp.dot(before, hot0.astype(bf16), preferred_element_type=f32)
        count1 = jnp.dot(before, hot1.astype(bf16), preferred_element_type=f32)
        count1 = count1 + jnp.sum(hot0, axis=0, keepdims=True)
        rank0 = jnp.sum(count0 * hot0, axis=1, keepdims=True)
        rank1 = jnp.sum(count1 * hot1, axis=1, keepdims=True)
        slots = lax.broadcasted_iota(jnp.int32, (TOK, N_DEV * CAP), 1)

        def place(e):
            return (((e & 3) + ((e >> 3) & 3) + (e >> 5)) & 3) * 32 + (e >> 2)

        c0 = (slots == place(r0) * CAP + rank0.astype(jnp.int32)).astype(f32)
        c1 = (slots == place(r1) * CAP + rank1.astype(jnp.int32)).astype(f32)
        pick_ref[:TOK] = c0.astype(bf16)
        pick_ref[TOK:] = c1.astype(bf16)
        picked = lax.dot_general(
            (c0 + c1).astype(bf16), normed, (((0,), (0,)), ((), ())), preferred_element_type=f32
        ).astype(bf16)
        rows_ref[...] = picked.reshape(N_DEV, CAP, D)
        l0, l1 = lg_ref[0:1], lg_ref[1:2]
        top = jnp.maximum(l0, l1)
        e0, e1 = jnp.exp(l0 - top), jnp.exp(l1 - top)
        w_ref[:, 0:1] = column(gp_ref[...] * (e0 / (e0 + e1)))
        w_ref[:, 1:2] = column(gp_ref[...] * (e1 / (e0 + e1)))
        arrived[me] = rows_ref[me]

    def dispatch(jd, first, last):
        def send(m, _):
            k = (m * 11) % 32
            z2, y2, c2 = (z + k // 8) % 4, (y + (k // 2) % 4) % 4, (c + k % 2) % 2
            x2 = (g + jd + 8 - y2 - z2) % 4
            e2 = (z2 * 4 + y2) * 2 + c2
            remote(
                rows_ref.at[((g + jd) % 4) * 32 + e2], arrived.at[me],
                disp_send, disp_recv.at[(4 - jd) % 4], (e2, x2),
            ).start()
            return 0

        lax.fori_loop(first, last, send, 0)

    def experts(j):
        count = 31 if j == 0 else 32
        span = pl.ds(0, count)
        remote(
            rows_ref.at[span], arrived.at[span], disp_send, disp_recv.at[j], (partner, tp)
        ).wait_recv()
        group = (g + j) % 4
        at = pl.ds(pl.multiple_of(group * 32, 32), 32)
        x = arrived[at].reshape(32 * CAP, D)
        gate = jnp.dot(x, wg[...], preferred_element_type=f32)
        up = jnp.dot(x, wu[...], preferred_element_type=f32)
        hidden = (gate / (1.0 + jnp.exp(-gate)) * up).astype(bf16)
        out = jnp.dot(hidden, wd[...], preferred_element_type=f32).astype(bf16)
        sent[at] = out.reshape(32, CAP, D)

    def give_back(j):
        if j == 0:
            ret[me] = sent[me]

        def send(m, _):
            k = (m * 11) % 32
            z2, y2, c2 = (z + k // 8) % 4, (y + (k // 2) % 4) % 4, (c + k % 2) % 2
            x2 = (g + j + 8 - y2 - z2) % 4
            e2 = (z2 * 4 + y2) * 2 + c2
            remote(
                sent.at[((g + j) % 4) * 32 + e2], ret.at[me],
                ret_send, ret_recv.at[(4 - j) % 4], (e2, x2),
            ).start()
            return 0

        lax.fori_loop(1 if j == 0 else 0, 32, send, 0)

    def combine(j):
        count = 31 if j == 0 else 32
        span = pl.ds(0, count)
        remote(
            sent.at[span], ret.at[span], ret_send, ret_recv.at[j], (partner, tp)
        ).wait_recv()
        group = (g + j) % 4
        back = ret[pl.ds(pl.multiple_of(group * 32, 32), 32)].reshape(32 * CAP, D)
        pick = pick_ref[:, pl.ds(pl.multiple_of(group * 128, 128), 128)]
        picked = jnp.dot(pick, back, preferred_element_type=f32)
        part = picked[:TOK] * w_ref[:, 0:1] + picked[TOK:] * w_ref[:, 1:2]
        if j == 0:
            b_sum[...] = part
        else:
            b_sum[...] += part

    ones = jnp.ones((KEY_BLOCK, HD), bf16)

    def attend(dz):
        if dz == 0:
            for p in (0, 1):
                to_partner(p, 0, 0, None, len(ARRIVALS) + p).wait_recv()
        for a in ARRIVALS:
            if (a[2] if a[0] == 0 else a[1]) == dz:
                to_partner(*a, SEM_OF[a]).wait_recv()
        plane = ((z + dz + 4) % 4) * (8 * ROWS)

        def block(i, _):
            at = pl.ds(pl.multiple_of(plane + i * KEY_BLOCK, KEY_BLOCK), KEY_BLOCK)
            key = kvbuf[at, :HD]
            value = jnp.concatenate([kvbuf[at, HD:], ones], axis=1)
            for t in range(4):
                rows = pl.ds(t * 256, 256)
                s = lax.dot_general(
                    qr_ref[rows], key, (((1,), (1,)), ((), ())), preferred_element_type=f32
                )
                weights = jnp.exp2(s * SCALE_LOG2E).astype(bf16)
                acc[rows] += jnp.dot(weights, value, preferred_element_type=f32)
            return 0

        lax.fori_loop(0, 8 * ROWS // KEY_BLOCK, block, 0)

    start_own()
    for step in (0, 1):
        pl.semaphore_wait(round_sem.at[step], len(kin))
        tell(round_sem.at[step + 1])
    for load in loads:
        load.start()
    pick_rows()
    pl.semaphore_wait(round_sem.at[2], len(kin))
    for kind, at in SCHEDULE:
        if kind == "queries":
            for take in takes[7:9]:
                take.wait()
            qr_ref[:ROWS] = turned(q_ref[:, :HD], qg_ref[...])
            qr_ref[ROWS:] = turned(q_ref[:, HD:], qg_ref[...])
            acc[...] = jnp.zeros_like(acc)
        elif kind == "rows":
            dispatch((4 - at) % 4, 1 if at == 0 else 0, 32)
        elif kind == "relay":
            for a in ARRIVALS:
                if abs(a[1]) + abs(a[2]) == at:
                    relay(a)
        elif kind == "experts":
            if at == 0:
                for load in loads[:3]:
                    load.wait()
            experts(at)
            give_back(at)
        else:
            attend(at)

    for t in range(4):
        for h in range(2):
            part = acc[pl.ds(h * ROWS + t * TOK, TOK)]
            att_out[t, :, h * HD : (h + 1) * HD] = (part[:, :HD] / part[:, HD:]).astype(bf16)
    for step in (1, 2, 3):
        to = (tp + step) % 4
        remote(att_out.at[to], att_in.at[tp], att_send, att_recv, (ep, to)).start()
    att_in[tp] = att_out[tp]
    for j in (0, 3, 2):
        combine(j)
    loads[3].wait()
    span = pl.ds(0, 3)
    remote(att_out.at[span], att_in.at[span], att_send, att_recv, (partner, tp)).wait_recv()
    total = jnp.dot(att_in[0], op[0:256], preferred_element_type=f32)
    for t in range(1, 4):
        total += jnp.dot(att_in[t], op[t * 256 : (t + 1) * 256], preferred_element_type=f32)
    a_buf[...] = total.astype(bf16)
    out_a = pltpu.make_async_copy(a_buf, a_hbm, w_sem.at[4])
    out_a.start()
    combine(1)
    b_buf[...] = b_sum[...].astype(bf16)
    out_b = pltpu.make_async_copy(b_buf, b_hbm, w_sem.at[5])
    out_b.start()
    span = pl.ds(0, N_DEV - 1)

    remote(
        rows_ref.at[span], arrived.at[span], disp_send, ret_recv.at[0], (partner, tp)
    ).wait_send()
    remote(sent.at[span], ret.at[span], ret_send, ret_recv.at[0], (partner, tp)).wait_send()
    remote(
        kvbuf.at[pl.ds(0, 15 * ROWS)], kvbuf.at[pl.ds(0, 15 * ROWS)],
        kv_send, kv_recv.at[0], (partner, tp),
    ).wait_send()
    remote(
        kvbuf.at[pl.ds(0, 16 * ROWS)], kvbuf.at[pl.ds(0, 16 * ROWS)],
        d2d_send, d2d_recv.at[0], (partner, tp),
    ).wait_send()
    three = pl.ds(0, 3)
    remote(att_out.at[three], att_in.at[three], att_send, att_recv, (partner, tp)).wait_send()
    out_a.wait()
    out_b.wait()


def final_kernel(a_in, b_in, a_out, b_out, held, sem):
    ins = [pltpu.make_async_copy(x, held.at[i], sem.at[i]) for i, x in enumerate((a_in, b_in))]
    outs = [
        pltpu.make_async_copy(held.at[i], x, sem.at[2 + i]) for i, x in enumerate((a_out, b_out))
    ]
    for copy in ins:
        copy.start()
    for i in (0, 1):
        ins[i].wait()
        outs[i].start()
    for copy in outs:
        copy.wait()


def body(
    queries, keys, values, query_gain, key_gain, out_proj, tokens_b, norm_gain, routes,
    group_prob, expert_logits, w_gate, w_up, w_down,
):
    bf16, f32 = jnp.bfloat16, jnp.float32
    tables = [jnp.asarray(t) for t in angle_tables()]
    out, buf = jax.ShapeDtypeStruct, pltpu.VMEM
    dma, many = pltpu.SemaphoreType.DMA, len(ARRIVALS)
    mixed = pl.pallas_call(
        main_kernel,
        out_shape=(out((TOK, D), bf16), out((TOK, D), bf16)),
        in_specs=[ANY] * 18,
        out_specs=(HBM, HBM),
        scratch_shapes=[
            buf((ROWS, 2 * HD), bf16), buf((ROWS, HD), bf16), buf((1, HD), f32), buf((1, HD), f32),
            buf((ROWS // GRID_W, HD), f32), buf((ROWS // GRID_W, HD), f32),
            buf((GRID_W, HD), f32), buf((GRID_W, HD), f32),
            buf((TOK, D), bf16), buf((1, D), f32), buf((2, TOK), jnp.int32), buf((1, TOK), f32),
            buf((2, TOK), f32),
            buf((N_DEV, CAP, D), bf16), buf((2 * ROWS, HD), bf16),
            buf((2 * TOK, N_DEV * CAP), bf16), buf((TOK, 2), f32),
            buf((TOK, D), bf16), buf((TOK, D), bf16), buf((TOK, D), f32),
            buf((SEQ, 2 * HD), bf16),
            buf((N_DEV, CAP, D), bf16), buf((N_DEV, CAP, D), bf16), buf((N_DEV, CAP, D), bf16),
            buf((2 * ROWS, 2 * HD), f32),
            buf((4, TOK, 2 * HD), bf16), buf((4, TOK, 2 * HD), bf16),
            buf((D, FF), bf16), buf((D, FF), bf16), buf((FF, D), bf16), buf((8 * HD, D), bf16),
            dma((6,)), dma((14,)), dma, dma((4,)), dma, dma((4,)),
            dma, dma((many,)), dma, dma((many + 2,)), dma, dma,
            pltpu.SemaphoreType.REGULAR((3,)),
        ],
        compiler_params=pltpu.CompilerParams(
            collective_id=0, has_side_effects=True, vmem_limit_bytes=60 << 20
        ),
    )(
        queries, keys, values, query_gain.reshape(1, HD), key_gain.reshape(1, HD), *tables,
        tokens_b, norm_gain.reshape(1, D), routes.T, group_prob.reshape(1, TOK),
        expert_logits.T, w_gate, w_up, w_down, out_proj,
    )
    return pl.pallas_call(
        final_kernel,
        out_shape=(out((TOK, D), bf16), out((TOK, D), bf16)),
        in_specs=[HBM] * 2,
        out_specs=(HBM,) * 2,
        scratch_shapes=[buf((2, TOK, D), bf16), dma((4,))],
        compiler_params=pltpu.CompilerParams(vmem_limit_bytes=60 << 20),
    )(*mixed)


def solution(mesh):
    both = P(("ep", "tp"), None)
    placed = (
        P("ep", "tp"),
        P("ep", "tp"),
        P("ep", "tp"),
        P(),
        P(),
        P(),
        both,
        P(),
        both,
        P(("ep", "tp")),
        both,
        P(("ep", "tp"), None, None),
        P(("ep", "tp"), None, None),
        P(("ep", "tp"), None, None),
    )
    return jax.shard_map(
        body, mesh=mesh, in_specs=placed, out_specs=(both, both), check_vma=False
    )
```

```python
import functools

import jax
import jax.numpy as jnp
import numpy as np
from jax import lax
from jax.experimental import pallas as pl
from jax.experimental.pallas import tpu as pltpu
from jax.sharding import PartitionSpec as P

GRID_W = 64
NORM_EPS = 1e-06
ROPE_BASE = 10000.0
HD = 128
CAP = 4
N_DEV = 128
ROWS = 512
TOK = 128
D = 2048
FF = 512
SEQ = 16384
SCALE_LOG2E = float(HD**-0.5 * np.log2(np.e))
KEY_BLOCK = 2048
MESH = pl.DeviceIdType.MESH
VMEM = pl.BlockSpec(memory_space=pltpu.VMEM)
ANY = pl.BlockSpec(memory_space=pl.ANY)
HBM = pl.BlockSpec(memory_space=pltpu.HBM)


def angle_tables():
    quarter = HD // 4
    freq = (ROPE_BASE ** (-np.arange(quarter, dtype=np.float64) / quarter)).astype(np.float32)

    def pair(count, at):
        angles = np.arange(count, dtype=np.float32)[:, None] * freq[None, :]
        cos = np.zeros((count, HD), np.float32)
        sin = np.zeros((count, HD), np.float32)
        c, s = np.cos(angles.astype(np.float64)), np.sin(angles.astype(np.float64))
        cos[:, at : at + quarter] = c
        cos[:, 64 + at : 64 + at + quarter] = c
        sin[:, at : at + quarter] = -s
        sin[:, 64 + at : 64 + at + quarter] = s
        return cos, sin

    return pair(SEQ // GRID_W, 0) + pair(GRID_W, quarter)


def arrivals():
    def of(o1, o2):
        parts = (0, 1) if (o1 == 2 or o2 == 2) else (None,)
        return [(p, o1, o2, part) for p in (0, 1) for part in parts]

    order = []
    for o1, o2 in [
        (-1, 0), (1, 0), (0, -1), (0, 1), (2, 0),
        (-1, -1), (1, 1), (-1, 1), (1, -1), (0, 2),
        (2, -1), (2, 1), (-1, 2), (1, 2), (2, 2),
    ]:
        order += of(o1, o2)
    return order


ARRIVALS = arrivals()
SEM_OF = {a: i for i, a in enumerate(ARRIVALS)}

SCHEDULE = (
    ("rows", 0),
    ("relay", 1),
    ("rows", 1),
    ("relay", 2),
    ("rows", 2),
    ("queries", 0),
    ("relay", 3),
    ("rows", 3),
    ("attend", 0),
    ("relay", 4),
    ("experts", 0),
    ("experts", 1),
    ("attend", 1),
    ("experts", 2),
    ("experts", 3),
    ("attend", -1),
    ("attend", 2),
)


def main_kernel(
    q_hbm, k_hbm, v_hbm, qg_hbm, kg_hbm, rc_hbm, rs_hbm, cc_hbm, cs_hbm,
    tok_hbm, ng_hbm, routes_hbm, gp_hbm, lg_hbm, wg_hbm, wu_hbm, wd_hbm, op_hbm,
    a_hbm, b_hbm,
    q_ref, k_ref, qg_ref, kg_ref, rc_ref, rs_ref, cc_ref, cs_ref,
    tok_ref, ng_ref, routes_ref, gp_ref, lg_ref,
    rows_ref, qr_ref, pick_ref, w_ref, a_buf, b_buf, b_sum,
    kvbuf, arrived, sent, ret, acc, att_out, att_in, wg, wu, wd, op,
    w_sem, in_sem, disp_send, disp_recv, ret_send, ret_recv,
    kv_send, kv_recv, d2d_send, d2d_recv, att_send, att_recv, round_sem,
):
    f32, bf16 = jnp.float32, jnp.bfloat16
    ep, tp = lax.axis_index("ep"), lax.axis_index("tp")
    z, y, c = ep // 8, (ep // 2) % 4, ep % 2
    g = (tp + y + z) % 4
    me = g * 32 + ep
    partner = ep + 1 - 2 * c
    own_rows = pl.ds(pl.multiple_of(ep * ROWS, ROWS), ROWS)
    grid_rows = ROWS // GRID_W
    here = pl.ds(pl.multiple_of(ep * grid_rows, grid_rows), grid_rows)

    barrier = pltpu.get_barrier_semaphore()

    kin = [(ep, (tp + step) % 4) for step in (1, 3, 2)]
    kin += [((z * 4 + (y + step) % 4) * 2 + c, tp) for step in (1, 3, 2)]
    kin += [((((z + step) % 4) * 4 + y) * 2 + c, tp) for step in (1, 3, 2)]
    kin += [(partner, tp)]

    def tell(sem):
        for to in kin:
            pl.semaphore_signal(sem, 1, device_id=to, device_id_type=MESH)

    def next_round(step):
        pl.semaphore_wait(round_sem.at[step], len(kin))
        tell(round_sem.at[step + 1])

    tell(barrier)

    takes = [
        (k_hbm, k_ref), (kg_hbm, kg_ref), (rc_hbm.at[here], rc_ref), (rs_hbm.at[here], rs_ref),
        (cc_hbm, cc_ref), (cs_hbm, cs_ref), (v_hbm, kvbuf.at[own_rows, pl.ds(HD, HD)]),
        (q_hbm, q_ref), (qg_hbm, qg_ref),
        (tok_hbm, tok_ref), (ng_hbm, ng_ref), (routes_hbm, routes_ref), (gp_hbm, gp_ref),
        (lg_hbm, lg_ref),
    ]
    takes = [pltpu.make_async_copy(x, to, in_sem.at[i]) for i, (x, to) in enumerate(takes)]
    for take in takes:
        take.start()

    loads = [
        pltpu.make_async_copy(wg_hbm.at[0], wg, w_sem.at[0]),
        pltpu.make_async_copy(wu_hbm.at[0], wu, w_sem.at[1]),
        pltpu.make_async_copy(wd_hbm.at[0], wd, w_sem.at[2]),
        pltpu.make_async_copy(op_hbm, op, w_sem.at[3]),
    ]
    def remote(src, dst, send, recv, to):
        return pltpu.make_async_remote_copy(
            src_ref=src, dst_ref=dst, send_sem=send, recv_sem=recv,
            device_id=to, device_id_type=MESH,
        )

    for take in takes[:7]:
        take.wait()
    cos = (rc_ref[...][:, None, :] + cc_ref[...][None, :, :]).reshape(ROWS, HD)
    sin = (rs_ref[...][:, None, :] + cs_ref[...][None, :, :]).reshape(ROWS, HD)

    def turned(x, gain):
        x = x.astype(f32)
        x = x * lax.rsqrt(jnp.mean(x * x, axis=-1, keepdims=True) + NORM_EPS) * gain
        return (x * cos + pltpu.roll(x, 64, 1) * sin).astype(bf16)

    kvbuf[own_rows, :HD] = turned(k_ref[...], kg_ref[...])
    pl.semaphore_wait(barrier, len(kin))
    tell(round_sem.at[0])

    def moved(p, ring, step):
        if (ring == 0) == (p == 0):
            return ((z * 4 + (y + step + 4) % 4) * 2 + c, tp)
        return ((((z + step + 4) % 4) * 4 + y) * 2 + c, tp)

    def owner_rows(p, o1, o2, part):
        dy, dz = (o1, o2) if p == 0 else (o2, o1)
        owner = (((z + dz + 4) % 4) * 4 + (y + dy + 4) % 4) * 2 + c
        start = owner * ROWS + p * 256 + (0 if part is None else part * 128)
        size = 256 if part is None else 128
        return pl.ds(pl.multiple_of(start, 128), size)

    def kv_copy(p, o1, o2, part, arrival, to):
        at = kvbuf.at[owner_rows(p, o1, o2, part)]
        return remote(at, at, kv_send, kv_recv.at[SEM_OF[arrival]], to)

    def to_partner(p, o1, o2, part, sem):
        at = kvbuf.at[owner_rows(p, o1, o2, part)]
        return remote(at, at, d2d_send, d2d_recv.at[sem], (partner, tp))

    def start_own():
        for p in (0, 1):
            for ring in (0, 1):
                for step in (1, -1):
                    arrival = (p, -step, 0, None) if ring == 0 else (p, 0, -step, None)
                    kv_copy(p, 0, 0, None, arrival, moved(p, ring, step)).start()
        for p in (0, 1):
            to_partner(p, 0, 0, None, len(ARRIVALS) + p).start()

    def relay(a):
        p, o1, o2, part = a
        kv_copy(p, o1, o2, part, a, (partner, tp)).wait_recv()
        if o2 == 0 and o1 in (-1, 1):
            half = 0 if o1 == -1 else 1
            kv_copy(p, o1, 0, half, (p, 2, 0, half), moved(p, 0, -o1)).start()
        if o2 == 0:
            for step in (1, -1):
                kv_copy(p, o1, 0, part, (p, o1, -step, part), moved(p, 1, step)).start()
        if o2 in (-1, 1):
            half = 0 if o2 == -1 else 1
            if part is None or part == half:
                kv_copy(p, o1, o2, half, (p, o1, 2, half), moved(p, 1, -o2)).start()
        to_partner(p, o1, o2, part, SEM_OF[a]).start()

    def pick_rows():
        for take in takes[9:]:
            take.wait()
        lane = lax.broadcasted_iota(jnp.int32, (TOK, N_DEV), 1)
        sub = lax.broadcasted_iota(jnp.int32, (TOK, N_DEV), 0)
        diagonal = sub == lane

        def column(row):
            return jnp.sum(jnp.where(diagonal, row, 0.0), axis=1, keepdims=True)

        wide = tok_ref[...].astype(f32)
        normed = (
            wide * lax.rsqrt(jnp.mean(wide * wide, axis=-1, keepdims=True) + NORM_EPS) * ng_ref[...]
        ).astype(bf16)
        routed = routes_ref[...].astype(f32)
        r0 = column(routed[0:1]).astype(jnp.int32)
        r1 = column(routed[1:2]).astype(jnp.int32)
        hot0 = (lane == r0).astype(f32)
        hot1 = (lane == r1).astype(f32)
        before = (sub > lane).astype(f32).astype(bf16)
        count0 = jnp.dot(before, hot0.astype(bf16), preferred_element_type=f32)
        count1 = jnp.dot(before, hot1.astype(bf16), preferred_element_type=f32)
        count1 = count1 + jnp.sum(hot0, axis=0, keepdims=True)
        rank0 = jnp.sum(count0 * hot0, axis=1, keepdims=True)
        rank1 = jnp.sum(count1 * hot1, axis=1, keepdims=True)
        slots = lax.broadcasted_iota(jnp.int32, (TOK, N_DEV * CAP), 1)

        def place(e):
            return (((e & 3) + ((e >> 3) & 3) + (e >> 5)) & 3) * 32 + (e >> 2)

        c0 = (slots == place(r0) * CAP + rank0.astype(jnp.int32)).astype(f32)
        c1 = (slots == place(r1) * CAP + rank1.astype(jnp.int32)).astype(f32)
        pick_ref[:TOK] = c0.astype(bf16)
        pick_ref[TOK:] = c1.astype(bf16)
        next_round(1)
        picked = lax.dot_general(
            (c0 + c1).astype(bf16), normed, (((0,), (0,)), ((), ())), preferred_element_type=f32
        ).astype(bf16)
        rows_ref[...] = picked.reshape(N_DEV, CAP, D)
        l0, l1 = lg_ref[0:1], lg_ref[1:2]
        top = jnp.maximum(l0, l1)
        e0, e1 = jnp.exp(l0 - top), jnp.exp(l1 - top)
        w_ref[:, 0:1] = column(gp_ref[...] * (e0 / (e0 + e1)))
        w_ref[:, 1:2] = column(gp_ref[...] * (e1 / (e0 + e1)))
        arrived[me] = rows_ref[me]

    def dispatch(jd, first, last):
        def send(m, _):
            k = (m * 11) % 32
            z2, y2, c2 = (z + k // 8) % 4, (y + (k // 2) % 4) % 4, (c + k % 2) % 2
            x2 = (g + jd + 8 - y2 - z2) % 4
            e2 = (z2 * 4 + y2) * 2 + c2
            remote(
                rows_ref.at[((g + jd) % 4) * 32 + e2], arrived.at[me],
                disp_send, disp_recv.at[(4 - jd) % 4], (e2, x2),
            ).start()
            return 0

        lax.fori_loop(first, last, send, 0)

    def experts(j):
        count = 31 if j == 0 else 32
        span = pl.ds(0, count)
        remote(
            rows_ref.at[span], arrived.at[span], disp_send, disp_recv.at[j], (partner, tp)
        ).wait_recv()
        group = (g + j) % 4
        at = pl.ds(pl.multiple_of(group * 32, 32), 32)
        x = arrived[at].reshape(32 * CAP, D)
        gate = jnp.dot(x, wg[...], preferred_element_type=f32)
        up = jnp.dot(x, wu[...], preferred_element_type=f32)
        hidden = (gate / (1.0 + jnp.exp(-gate)) * up).astype(bf16)
        out = jnp.dot(hidden, wd[...], preferred_element_type=f32).astype(bf16)
        sent[at] = out.reshape(32, CAP, D)

    def give_back(j):
        if j == 0:
            ret[me] = sent[me]

        def send(m, _):
            k = (m * 11) % 32
            z2, y2, c2 = (z + k // 8) % 4, (y + (k // 2) % 4) % 4, (c + k % 2) % 2
            x2 = (g + j + 8 - y2 - z2) % 4
            e2 = (z2 * 4 + y2) * 2 + c2
            remote(
                sent.at[((g + j) % 4) * 32 + e2], ret.at[me],
                ret_send, ret_recv.at[(4 - j) % 4], (e2, x2),
            ).start()
            return 0

        lax.fori_loop(1 if j == 0 else 0, 32, send, 0)

    def combine(j):
        count = 31 if j == 0 else 32
        span = pl.ds(0, count)
        remote(
            sent.at[span], ret.at[span], ret_send, ret_recv.at[j], (partner, tp)
        ).wait_recv()
        group = (g + j) % 4
        back = ret[pl.ds(pl.multiple_of(group * 32, 32), 32)].reshape(32 * CAP, D)
        pick = pick_ref[:, pl.ds(pl.multiple_of(group * 128, 128), 128)]
        picked = jnp.dot(pick, back, preferred_element_type=f32)
        part = picked[:TOK] * w_ref[:, 0:1] + picked[TOK:] * w_ref[:, 1:2]
        if j == 0:
            b_sum[...] = part
        else:
            b_sum[...] += part

    ones = jnp.ones((KEY_BLOCK, HD), bf16)

    def attend(dz):
        if dz == 0:
            for p in (0, 1):
                to_partner(p, 0, 0, None, len(ARRIVALS) + p).wait_recv()
        for a in ARRIVALS:
            if (a[2] if a[0] == 0 else a[1]) == dz:
                to_partner(*a, SEM_OF[a]).wait_recv()
        plane = ((z + dz + 4) % 4) * (8 * ROWS)

        def block(i, _):
            at = pl.ds(pl.multiple_of(plane + i * KEY_BLOCK, KEY_BLOCK), KEY_BLOCK)
            key = kvbuf[at, :HD]
            value = jnp.concatenate([kvbuf[at, HD:], ones], axis=1)
            for t in range(4):
                rows = pl.ds(t * 256, 256)
                s = lax.dot_general(
                    qr_ref[rows], key, (((1,), (1,)), ((), ())), preferred_element_type=f32
                )
                weights = jnp.exp2(s * SCALE_LOG2E).astype(bf16)
                acc[rows] += jnp.dot(weights, value, preferred_element_type=f32)
            return 0

        lax.fori_loop(0, 8 * ROWS // KEY_BLOCK, block, 0)

    start_own()
    for load in loads:
        load.start()
    next_round(0)
    pick_rows()
    pl.semaphore_wait(round_sem.at[2], len(kin))
    for kind, at in SCHEDULE:
        if kind == "queries":
            for take in takes[7:9]:
                take.wait()
            qr_ref[:ROWS] = turned(q_ref[:, :HD], qg_ref[...])
            qr_ref[ROWS:] = turned(q_ref[:, HD:], qg_ref[...])
            acc[...] = jnp.zeros_like(acc)
        elif kind == "rows":
            dispatch((4 - at) % 4, 1 if at == 0 else 0, 32)
        elif kind == "relay":
            for a in ARRIVALS:
                if abs(a[1]) + abs(a[2]) == at:
                    relay(a)
        elif kind == "experts":
            if at == 0:
                for load in loads[:3]:
                    load.wait()
            experts(at)
            give_back(at)
        else:
            attend(at)

    for t in range(4):
        for h in range(2):
            part = acc[pl.ds(h * ROWS + t * TOK, TOK)]
            att_out[t, :, h * HD : (h + 1) * HD] = (part[:, :HD] / part[:, HD:]).astype(bf16)
    for step in (1, 2, 3):
        to = (tp + step) % 4
        remote(att_out.at[to], att_in.at[tp], att_send, att_recv, (ep, to)).start()
    att_in[tp] = att_out[tp]
    for j in (0, 3, 2):
        combine(j)
    loads[3].wait()
    span = pl.ds(0, 3)
    remote(att_out.at[span], att_in.at[span], att_send, att_recv, (partner, tp)).wait_recv()
    total = jnp.dot(att_in[0], op[0:256], preferred_element_type=f32)
    for t in range(1, 4):
        total += jnp.dot(att_in[t], op[t * 256 : (t + 1) * 256], preferred_element_type=f32)
    a_buf[...] = total.astype(bf16)
    out_a = pltpu.make_async_copy(a_buf, a_hbm, w_sem.at[4])
    out_a.start()
    combine(1)
    b_buf[...] = b_sum[...].astype(bf16)
    out_b = pltpu.make_async_copy(b_buf, b_hbm, w_sem.at[5])
    out_b.start()
    span = pl.ds(0, N_DEV - 1)

    remote(
        rows_ref.at[span], arrived.at[span], disp_send, ret_recv.at[0], (partner, tp)
    ).wait_send()
    remote(sent.at[span], ret.at[span], ret_send, ret_recv.at[0], (partner, tp)).wait_send()
    remote(
        kvbuf.at[pl.ds(0, 15 * ROWS)], kvbuf.at[pl.ds(0, 15 * ROWS)],
        kv_send, kv_recv.at[0], (partner, tp),
    ).wait_send()
    remote(
        kvbuf.at[pl.ds(0, 16 * ROWS)], kvbuf.at[pl.ds(0, 16 * ROWS)],
        d2d_send, d2d_recv.at[0], (partner, tp),
    ).wait_send()
    three = pl.ds(0, 3)
    remote(att_out.at[three], att_in.at[three], att_send, att_recv, (partner, tp)).wait_send()
    out_a.wait()
    out_b.wait()


def final_kernel(a_in, b_in, a_out, b_out, held, sem):
    ins = [pltpu.make_async_copy(x, held.at[i], sem.at[i]) for i, x in enumerate((a_in, b_in))]
    outs = [
        pltpu.make_async_copy(held.at[i], x, sem.at[2 + i]) for i, x in enumerate((a_out, b_out))
    ]
    for copy in ins:
        copy.start()
    for i in (0, 1):
        ins[i].wait()
        outs[i].start()
    for copy in outs:
        copy.wait()


def body(
    queries, keys, values, query_gain, key_gain, out_proj, tokens_b, norm_gain, routes,
    group_prob, expert_logits, w_gate, w_up, w_down,
):
    bf16, f32 = jnp.bfloat16, jnp.float32
    tables = [jnp.asarray(t) for t in angle_tables()]
    out, buf = jax.ShapeDtypeStruct, pltpu.VMEM
    dma, many = pltpu.SemaphoreType.DMA, len(ARRIVALS)
    mixed = pl.pallas_call(
        main_kernel,
        out_shape=(out((TOK, D), bf16), out((TOK, D), bf16)),
        in_specs=[ANY] * 18,
        out_specs=(HBM, HBM),
        scratch_shapes=[
            buf((ROWS, 2 * HD), bf16), buf((ROWS, HD), bf16), buf((1, HD), f32), buf((1, HD), f32),
            buf((ROWS // GRID_W, HD), f32), buf((ROWS // GRID_W, HD), f32),
            buf((GRID_W, HD), f32), buf((GRID_W, HD), f32),
            buf((TOK, D), bf16), buf((1, D), f32), buf((2, TOK), jnp.int32), buf((1, TOK), f32),
            buf((2, TOK), f32),
            buf((N_DEV, CAP, D), bf16), buf((2 * ROWS, HD), bf16),
            buf((2 * TOK, N_DEV * CAP), bf16), buf((TOK, 2), f32),
            buf((TOK, D), bf16), buf((TOK, D), bf16), buf((TOK, D), f32),
            buf((SEQ, 2 * HD), bf16),
            buf((N_DEV, CAP, D), bf16), buf((N_DEV, CAP, D), bf16), buf((N_DEV, CAP, D), bf16),
            buf((2 * ROWS, 2 * HD), f32),
            buf((4, TOK, 2 * HD), bf16), buf((4, TOK, 2 * HD), bf16),
            buf((D, FF), bf16), buf((D, FF), bf16), buf((FF, D), bf16), buf((8 * HD, D), bf16),
            dma((6,)), dma((14,)), dma, dma((4,)), dma, dma((4,)),
            dma, dma((many,)), dma, dma((many + 2,)), dma, dma,
            pltpu.SemaphoreType.REGULAR((3,)),
        ],
        compiler_params=pltpu.CompilerParams(
            collective_id=0, has_side_effects=True, vmem_limit_bytes=60 << 20
        ),
    )(
        queries, keys, values, query_gain.reshape(1, HD), key_gain.reshape(1, HD), *tables,
        tokens_b, norm_gain.reshape(1, D), routes.T, group_prob.reshape(1, TOK),
        expert_logits.T, w_gate, w_up, w_down, out_proj,
    )
    return pl.pallas_call(
        final_kernel,
        out_shape=(out((TOK, D), bf16), out((TOK, D), bf16)),
        in_specs=[HBM] * 2,
        out_specs=(HBM,) * 2,
        scratch_shapes=[buf((2, TOK, D), bf16), dma((4,))],
        compiler_params=pltpu.CompilerParams(vmem_limit_bytes=60 << 20),
    )(*mixed)


def solution(mesh):
    both = P(("ep", "tp"), None)
    placed = (
        P("ep", "tp"),
        P("ep", "tp"),
        P("ep", "tp"),
        P(),
        P(),
        P(),
        both,
        P(),
        both,
        P(("ep", "tp")),
        both,
        P(("ep", "tp"), None, None),
        P(("ep", "tp"), None, None),
        P(("ep", "tp"), None, None),
    )
    return jax.shard_map(
        body, mesh=mesh, in_specs=placed, out_specs=(both, both), check_vma=False
    )
```
